32 devices in a mesh: fs: 4 (over z), rep: 4 (over y, x), tp: 2 (over core).
Axes of the slice: x: 2, y: 2, z: 4, core: 2. Of those that a mesh axis runs over, the one named last changes fastest.
Arguments:
- normed_input: bfloat16 [2048, 1024], P(('fs', 'rep')), may hold values from -6 to 6
- query_cotangent: bfloat16 [2048, 512], P(('fs', 'rep'), 'tp'), may hold values from -0.029907227 to 0.029907227
- value_cotangent: bfloat16 [2048, 1024], P(('fs', 'rep'), 'tp'), may hold values from -0.029907227 to 0.029907227
- query_basis: bfloat16 [1024, 128], replicated, may hold values from -0.1875 to 0.1875
- value_basis: bfloat16 [1024, 128], replicated, may hold values from -0.1875 to 0.1875
- query_weight: float32 [1024, 512], P(('fs', 'rep'), 'tp'), may hold values from -0.1875 to 0.1875
- value_weight: float32 [1024, 1024], P(('fs', 'rep'), 'tp'), may hold values from -0.1875 to 0.1875
- query_first: float32 [128, 512], P(('fs', 'rep'), 'tp'), may hold values from -6 to 6
- query_second: float32 [128, 512], P(('fs', 'rep'), 'tp'), may hold values from 0.25 to 4
- value_first: float32 [128, 1024], P(('fs', 'rep'), 'tp'), may hold values from -6 to 6
- value_second: float32 [128, 1024], P(('fs', 'rep'), 'tp'), may hold values from 0.25 to 4
Outputs:
- query_update: float32 [1024, 512], P(('fs', 'rep'), 'tp')
- value_update: float32 [1024, 1024], P(('fs', 'rep'), 'tp')
- query_weight_new: float32 [1024, 512], P(('fs', 'rep'), 'tp')
- value_weight_new: float32 [1024, 1024], P(('fs', 'rep'), 'tp')
- query_first_new: float32 [128, 512], P(('fs', 'rep'), 'tp')
- query_second_new: float32 [128, 512], P(('fs', 'rep'), 'tp')
- value_first_new: float32 [128, 1024], P(('fs', 'rep'), 'tp')
- value_second_new: float32 [128, 1024], P(('fs', 'rep'), 'tp')
- query_copy: bfloat16 [1024, 512], P(None, 'tp')
- value_copy: bfloat16 [1024, 1024], P(None, 'tp')
The draws below stay inside these ranges and needn't reach their ends.
All inputs are finite; a program needn't handle non-finite values.
Results may differ from the reference program's by a relative error of at most 0.001.
Values may be sent and summed in bfloat16 or wider, within the bound.
No kernel may reach another device: no remote copies, remote signals or barrier semaphores. Data moves between devices by JAX's collectives and lax.ppermute only.
A program may use at most 64 MiB of HBM per device.

```python
import math
import jax
import jax.numpy as jnp
from jax import lax

D = 1024
RANK = 128
QW = 512
VW = 1024
TOKENS = 2048


def block_levels(stream_key, shape, shards, smallest, top_value):
    gain = 1.0
    for dim, parts in shards:
        steps = jax.random.uniform(jax.random.fold_in(jax.random.fold_in(stream_key, 6), dim), (parts,), jnp.float32, smallest / len(shards), top_value / len(shards))
        gain = gain * jnp.repeat(jnp.exp(steps), shape[dim] // parts).reshape((-1,) + (1,) * (len(shape) - 1 - dim))
    return gain


def normal_values(key, extent, width, most, split=(), dtype=jnp.bfloat16):
    values = jax.random.normal(key, extent, jnp.float32) * width
    if len(split) > 0:
        values = block_levels(key, extent, split, -0.22, 0.18) * values
    return jnp.clip(values, min=-most, max=most).astype(dtype)


def setup_inputs(seed: int = 0) -> dict:
    arg_keys = jax.random.split(jax.random.key(seed), 12)
    normed_input = normal_values(arg_keys[0], (TOKENS, D), 1.0, 6.0, ((0, 16),))
    query_cotangent = normal_values(arg_keys[1], (TOKENS, QW), 0.005, 0.029907227, ((0, 16), (1, 2)))
    value_cotangent = normal_values(arg_keys[2], (TOKENS, VW), 0.005, 0.029907227, ((0, 16), (1, 2)))
    query_basis = normal_values(arg_keys[3], (D, RANK), D ** -0.5, 0.1875)
    value_basis = normal_values(arg_keys[4], (D, RANK), D ** -0.5, 0.1875)
    query_weight = normal_values(arg_keys[5], (D, QW), D ** -0.5, 0.1875, ((0, 16), (1, 2)), jnp.float32)
    value_weight = normal_values(arg_keys[6], (D, VW), D ** -0.5, 0.1875, ((0, 16), (1, 2)), jnp.float32)
    query_first = normal_values(arg_keys[7], (RANK, QW), 1.0, 6.0, ((0, 16), (1, 2)), jnp.float32)
    query_second = jnp.clip(jnp.exp(math.log(4.0) - 2.7725887 * jax.random.uniform(arg_keys[8], (RANK, QW), jnp.float32) ** block_levels(arg_keys[8], (RANK, QW), ((0, 16), (1, 2)), -0.2, 0.2)), 0.25, 4.0)
    value_first = normal_values(arg_keys[9], (RANK, VW), 1.0, 6.0, ((0, 16), (1, 2)), jnp.float32)
    value_second = jnp.clip(jnp.exp(math.log(4.0) - 2.7725887 * jax.random.uniform(arg_keys[10], (RANK, VW), jnp.float32) ** block_levels(arg_keys[10], (RANK, VW), ((0, 16), (1, 2)), -0.2, 0.2)), 0.25, 4.0)
    return dict(normed_input=normed_input, query_cotangent=query_cotangent, value_cotangent=value_cotangent, query_basis=query_basis, value_basis=value_basis, query_weight=query_weight, value_weight=value_weight, query_first=query_first, query_second=query_second, value_first=value_first, value_second=value_second)


def update_matrix(normed_input, cotangent, basis, weight, first_old, second_old):
    gradient = jnp.dot(normed_input.T, cotangent, preferred_element_type=jnp.float32)
    basis_wide = basis.astype(jnp.float32)
    projected = jnp.dot(basis_wide.T, gradient, precision=lax.Precision.HIGHEST)
    first_new = 0.9 * first_old + 0.1 * projected
    second_new = 0.99 * second_old + 0.01 * projected * projected
    direction = first_new / (jnp.sqrt(second_new) + 1e-08)
    norm_scale = jnp.sqrt(jnp.mean(direction * direction) + 1.0)
    update = jnp.dot(basis_wide, direction, precision=lax.Precision.HIGHEST) / norm_scale
    weight_new = weight - 0.01 * update
    return (update, weight_new, first_new, second_new, weight_new.astype(jnp.bfloat16))

def reference(normed_input, query_cotangent, value_cotangent, query_basis, value_basis, query_weight, value_weight, query_first, query_second, value_first, value_second):
    query_out = update_matrix(normed_input, query_cotangent, query_basis, query_weight, query_first, query_second)
    value_out = update_matrix(normed_input, value_cotangent, value_basis, value_weight, value_first, value_second)
    return (query_out[0], value_out[0], query_out[1], value_out[1], query_out[2], query_out[3], value_out[2], value_out[3], query_out[4], value_out[4])
```

```python
import functools

import jax
import jax.numpy as jnp
from jax import lax
from jax.experimental import pallas as pl
from jax.experimental.pallas import tpu as pltpu
from jax.sharding import PartitionSpec as P


def swap(block, axis, mask):
    count = lax.axis_size(axis)
    return lax.ppermute(block, axis, [(i, i ^ mask) for i in range(count)])


def spread(block, axis):
    return [block] + [swap(block, axis, k) for k in range(1, lax.axis_size(axis))]


def in_order(blocks, own):
    stacked = jnp.stack(blocks)
    return jnp.stack(
        [lax.dynamic_index_in_dim(stacked, j ^ own, 0, keepdims=False) for j in range(len(blocks))]
    )


def split_parts(wide):
    high_part = wide.astype(jnp.bfloat16)
    held = lax.optimization_barrier(high_part)
    low_part = (wide - held.astype(jnp.float32)).astype(jnp.bfloat16)
    return (high_part, low_part)


def parts_product(high_part, low_part, cotangent):
    dims = (((0,), (0,)), ((), ()))
    first_term = lax.dot_general(high_part, cotangent, dims, preferred_element_type=jnp.float32)
    second_term = lax.dot_general(low_part, cotangent, dims, preferred_element_type=jnp.float32)
    return first_term + second_term


def moments(projected, first_old, second_old):
    first_new = 0.9 * first_old + 0.1 * projected
    second_new = 0.99 * second_old + 0.01 * projected * projected
    return (first_new, second_new, first_new / (jnp.sqrt(second_new) + 1e-08))


def finish_kernel(
    counts,
    place,
    scale,
    direction,
    query_basis,
    value_basis,
    *refs,
):
    fs, rep, rows, query_width = counts
    query_blocks, value_blocks = refs[:fs], refs[fs : fs + rep]
    (
        query_update,
        value_update,
        query_new,
        value_new,
        query_copy,
        value_copy,
        query_product,
        value_product,
    ) = refs[fs + rep :]
    z, r = place[0], place[1]
    for basis, product, lo, hi in (
        (query_basis, query_product, 0, query_width),
        (value_basis, value_product, query_width, direction.shape[1]),
    ):
        wide = direction[:, lo:hi]
        high = wide.astype(jnp.bfloat16)
        low = (wide - high.astype(jnp.float32)).astype(jnp.bfloat16)
        product[...] = jnp.dot(
            basis[...], high, preferred_element_type=jnp.float32
        ) + jnp.dot(basis[...], low, preferred_element_type=jnp.float32)

    def emit(product, factor, block, part, update, new, copy, kz, kr):
        own = kz == 0 and kr == 0
        owner = (z ^ kz) * rep + (r ^ kr)
        where = pl.ds(pl.multiple_of(owner * rows, rows), rows)
        step = product[where, :] * factor
        weight = block[part * rows : (part + 1) * rows, :] - 0.01 * step
        copy[where, :] = weight.astype(jnp.bfloat16)
        if own:
            update[...] = step
            new[...] = weight

    for kz in range(fs):
        for kr in range(rep):
            emit(query_product, scale[0], query_blocks[kz], kr, query_update, query_new, query_copy, kz, kr)
            emit(value_product, scale[1], value_blocks[kr], kz, value_update, value_new, value_copy, kz, kr)


def body(
    normed_input,
    query_cotangent,
    value_cotangent,
    query_basis,
    value_basis,
    query_weight,
    value_weight,
    query_first,
    query_second,
    value_first,
    value_second,
):
    fs, rep, tp = lax.axis_size("fs"), lax.axis_size("rep"), lax.axis_size("tp")
    z, r = lax.axis_index("fs"), lax.axis_index("rep")
    rows = query_weight.shape[0]
    query_width, value_width = query_cotangent.shape[1], value_cotangent.shape[1]
    width = query_width + value_width
    ranks = query_first.shape[0]

    firsts = jnp.concatenate([query_first, value_first], axis=1)
    seconds = jnp.concatenate([query_second, value_second], axis=1)
    moment_rows = spread(jnp.concatenate([firsts, seconds], axis=0), "fs")
    value_z = spread(value_weight, "fs")
    query_r = spread(query_weight, "rep")

    reduced_query = jnp.dot(normed_input, query_basis, preferred_element_type=jnp.float32)
    reduced_value = jnp.dot(normed_input, value_basis, preferred_element_type=jnp.float32)
    partial = jnp.concatenate(
        [
            parts_product(*split_parts(reduced_query), query_cotangent),
            parts_product(*split_parts(reduced_value), value_cotangent),
        ],
        axis=1,
    ).reshape(fs, rep, ranks, width)

    def chunk(k):
        return lax.dynamic_slice_in_dim(partial, r ^ k, 1, 1).reshape(fs * ranks, width)

    summed = chunk(0)
    for k in range(1, rep):
        summed = summed + swap(chunk(k), "rep", k)
    step = 1
    while step < fs:
        summed = summed + swap(summed, "fs", step)
        step *= 2

    value_blocks = spread(jnp.concatenate(value_z, axis=0), "rep")
    query_blocks = spread(jnp.concatenate(query_r, axis=0), "fs")

    held = in_order(moment_rows, z)
    first_new, second_new, direction = moments(
        summed,
        held[:, :ranks].reshape(fs * ranks, width),
        held[:, ranks:].reshape(fs * ranks, width),
    )
    first_new = lax.dynamic_slice_in_dim(first_new, z * ranks, ranks, 0)
    second_new = lax.dynamic_slice_in_dim(second_new, z * ranks, ranks, 0)

    whole = in_order([d.reshape(fs, ranks, width) for d in spread(direction, "rep")], r)
    whole = whole.transpose(1, 0, 2, 3).reshape(fs * rep * ranks, width)
    squares = whole * whole
    sums = jnp.stack([jnp.sum(squares[:, :query_width]), jnp.sum(squares[:, query_width:])])
    if tp == 2:
        sums = sums + swap(sums, "tp", 1)
    else:
        sums = lax.psum(sums, "tp")
    entries = whole.shape[0] * tp * jnp.array([query_width, value_width], jnp.float32)
    factor = 1.0 / jnp.sqrt(sums / entries + 1.0)

    total = fs * rep * rows
    f32, bf16 = jnp.float32, jnp.bfloat16
    vmem = pl.BlockSpec(memory_space=pltpu.VMEM)
    smem = pl.BlockSpec(memory_space=pltpu.SMEM)
    if rows % 16 == 0 and query_width % 128 == 0 and value_width % 128 == 0:
        outs = pl.pallas_call(
            functools.partial(finish_kernel, (fs, rep, rows, query_width)),
            out_shape=(
                jax.ShapeDtypeStruct((rows, query_width), f32),
                jax.ShapeDtypeStruct((rows, value_width), f32),
                jax.ShapeDtypeStruct((rows, query_width), f32),
                jax.ShapeDtypeStruct((rows, value_width), f32),
                jax.ShapeDtypeStruct((total, query_width), bf16),
                jax.ShapeDtypeStruct((total, value_width), bf16),
            ),
            in_specs=[smem, smem] + [vmem] * (3 + fs + rep),
            out_specs=(vmem,) * 6,
            scratch_shapes=[
                pltpu.VMEM((total, query_width), f32),
                pltpu.VMEM((total, value_width), f32),
            ],
        )(
            jnp.stack([z, r]).astype(jnp.int32),
            factor,
            whole,
            query_basis,
            value_basis,
            *query_blocks,
            *value_blocks,
        )
        query_update, value_update, query_new, value_new, query_copy, value_copy = outs
    else:
        outs = []
        query_all = in_order([b.reshape(rep, rows, query_width) for b in query_blocks], z)
        query_all = jnp.stack([in_order(list(query_all[i]), r) for i in range(fs)])
        value_all = in_order([b.reshape(fs, rows, value_width) for b in value_blocks], r)
        value_all = jnp.stack([in_order(list(value_all[i]), z) for i in range(rep)], axis=1)
        for basis, weights, lo, hi, scale in (
            (query_basis, query_all, 0, query_width, factor[0]),
            (value_basis, value_all, query_width, width, factor[1]),
        ):
            update = scale * jnp.dot(
                basis.astype(f32), whole[:, lo:hi], precision=lax.Precision.HIGHEST
            )
            new = weights.reshape(total, hi - lo) - 0.01 * update
            place = (z * rep + r) * rows
            outs.append(lax.dynamic_slice_in_dim(update, place, rows, 0))
            outs.append(lax.dynamic_slice_in_dim(new, place, rows, 0))
            outs.append(new.astype(bf16))
        query_update, query_new, query_copy, value_update, value_new, value_copy = outs
    return (
        query_update,
        value_update,
        query_new,
        value_new,
        first_new[:, :query_width],
        second_new[:, :query_width],
        first_new[:, query_width:],
        second_new[:, query_width:],
        query_copy,
        value_copy,
    )


def solution(mesh):
    rows = P(("fs", "rep"), "tp")
    in_specs = (P(("fs", "rep"), None), rows, rows, P(), P()) + (rows,) * 6
    out_specs = (rows,) * 8 + (P(None, "tp"),) * 2
    return jax.shard_map(body, mesh=mesh, in_specs=in_specs, out_specs=out_specs, check_vma=False)
```

```python
import functools

import jax
import jax.numpy as jnp
from jax import lax
from jax.experimental import pallas as pl
from jax.experimental.pallas import tpu as pltpu
from jax.sharding import PartitionSpec as P


F32, BF16 = jnp.float32, jnp.bfloat16
VMEM = pl.BlockSpec(memory_space=pltpu.VMEM)
SMEM = pl.BlockSpec(memory_space=pltpu.SMEM)
ANY = pl.BlockSpec(memory_space=pltpu.MemorySpace.HBM)
PARAMS = pltpu.CompilerParams(vmem_limit_bytes=16 * 2**20)


def swap(block, axis, mask):
    count = lax.axis_size(axis)
    pairs = [(i, i ^ mask) for i in range(count)]
    return lax.ppermute(block, axis, pairs)


def spread(block, axis):
    return [block] + [swap(block, axis, k) for k in range(1, lax.axis_size(axis))]


def in_order(blocks, own):
    stacked = jnp.stack(blocks)
    return jnp.stack(
        [lax.dynamic_index_in_dim(stacked, j ^ own, 0, keepdims=False) for j in range(len(blocks))]
    )


def split_parts(wide):
    high_part = wide.astype(BF16)
    held = lax.optimization_barrier(high_part)
    low_part = (wide - held.astype(F32)).astype(BF16)
    return (high_part, low_part)


def parts_product(high_part, low_part, cotangent):
    dims = (((0,), (0,)), ((), ()))
    first_term = lax.dot_general(high_part, cotangent, dims, preferred_element_type=F32)
    second_term = lax.dot_general(low_part, cotangent, dims, preferred_element_type=F32)
    return first_term + second_term


def moments(projected, first_old, second_old):
    first_new = 0.9 * first_old + 0.1 * projected
    second_new = 0.99 * second_old + 0.01 * projected * projected
    return (first_new, second_new, first_new / (jnp.sqrt(second_new) + 1e-08))


def aligned(start, size):
    return pl.ds(pl.multiple_of(start * size, size), size)


def stage_kernel(query_weight, value_weight, query_first, value_first, *refs):
    query_second, value_second, weights, own, sems = refs
    rows, ranks = query_weight.shape[0], query_first.shape[0]
    query_width, width = query_weight.shape[1], weights.shape[1]
    copies = []
    for target, left, right, low in (
        (weights, query_weight, value_weight, 0),
        (own, query_weight, value_weight, 0),
        (own, query_first, value_first, rows),
        (own, query_second, value_second, rows + ranks),
    ):
        for source, columns in ((left, pl.ds(0, query_width)), (right, pl.ds(query_width, width - query_width))):
            copies.append(
                pltpu.make_async_copy(
                    source, target.at[pl.ds(low, source.shape[0]), columns], sems.at[len(copies)]
                )
            )
    for copy in copies:
        copy.start()
    for copy in copies:
        copy.wait()


def project_kernel(counts, place, *refs):
    fs, rep, ranks = counts
    sources, chunks, total = refs[:5], refs[5 : 5 + rep], refs[5 + rep]
    tokens, query_basis, value_basis, query_cot, value_cot = held = refs[6 + rep : 11 + rep]
    sems = refs[11 + rep]
    copies = [
        pltpu.make_async_copy(source, target, sems.at[i])
        for i, (source, target) in enumerate(zip(sources, held))
    ]
    for copy in copies:
        copy.start()
    for copy in copies:
        copy.wait()
    r = place[1]
    query_width = query_cot.shape[1]
    for basis, cot, lo in ((query_basis, query_cot, 0), (value_basis, value_cot, query_width)):
        reduced = jnp.dot(tokens[...], basis[...], preferred_element_type=F32)
        high = reduced.astype(BF16)
        low = (reduced - high.astype(F32)).astype(BF16)
        total[:, lo : lo + cot.shape[1]] = parts_product(high, low, cot[...])
    for k in range(rep):
        for zz in range(fs):
            chunks[k][zz * ranks : (zz + 1) * ranks, :] = total[
                aligned(zz * rep + (r ^ k), ranks), :
            ]


def moments_kernel(counts, place, mine, other, *refs):
    fs, rows, ranks, query_width = counts
    blocks, (query_first, query_second, value_first, value_second, direction) = refs[:fs], refs[fs:]
    z = place[0]
    for k in range(fs):
        where = aligned(z ^ k, ranks)
        first, second, ratio = moments(
            mine[where, :] + other[where, :],
            blocks[k][rows : rows + ranks, :],
            blocks[k][rows + ranks : rows + 2 * ranks, :],
        )
        direction[where, :] = ratio
        if k == 0:
            query_first[...] = first[:, :query_width]
            query_second[...] = second[:, :query_width]
            value_first[...] = first[:, query_width:]
            value_second[...] = second[:, query_width:]


def whole_kernel(counts, place, *refs):
    fs, rep, ranks, query_width = counts
    blocks, (whole, sums) = refs[:rep], refs[rep:]
    r = place[1]
    for k in range(rep):
        for zz in range(fs):
            whole[aligned(zz * rep + (r ^ k), ranks), :] = blocks[k][
                zz * ranks : (zz + 1) * ranks, :
            ]
    squares = whole[0:ranks, :] * whole[0:ranks, :]
    for row in range(1, fs * rep):
        part = whole[row * ranks : (row + 1) * ranks, :]
        squares = squares + part * part
    query_sum = jnp.sum(squares[:, :query_width], keepdims=True)
    value_sum = jnp.sum(squares[:, query_width:], keepdims=True)
    sums[0:1, :] = jnp.broadcast_to(query_sum, (1, sums.shape[1]))
    sums[1:2, :] = jnp.broadcast_to(value_sum, (1, sums.shape[1]))


def product_kernel(whole, query_basis, value_basis, query_product, value_product):
    query_width = query_product.shape[1]
    for basis, product, lo in (
        (query_basis, query_product, 0),
        (value_basis, value_product, query_width),
    ):
        wide = whole[:, lo : lo + product.shape[1]]
        high = wide.astype(BF16)
        low = (wide - high.astype(F32)).astype(BF16)
        product[...] = jnp.dot(basis[...], high, preferred_element_type=F32) + jnp.dot(
            basis[...], low, preferred_element_type=F32
        )


def finish_kernel(counts, place, sums, query_product, value_product, *refs):
    fs, rep, rows, entries = counts
    blocks = refs[: fs * rep]
    query_update, value_update, query_new, value_new, query_copy, value_copy = refs[fs * rep :]
    z, r = place[0], place[1]
    query_width = query_product.shape[1]
    query_scale = 1.0 / jnp.sqrt(sums[0:1, 0:1] / entries[0] + 1.0)
    value_scale = 1.0 / jnp.sqrt(sums[1:2, 0:1] / entries[1] + 1.0)
    for kz in range(fs):
        for kr in range(rep):
            where = aligned((z ^ kz) * rep + (r ^ kr), rows)
            held = blocks[kz * rep + kr]
            for product, scale, lo, update, new, copy in (
                (query_product, query_scale, 0, query_update, query_new, query_copy),
                (value_product, value_scale, query_width, value_update, value_new, value_copy),
            ):
                step = product[where, :] * scale
                weight = held[:, lo : lo + product.shape[1]] - 0.01 * step
                copy[where, :] = weight.astype(BF16)
                if kz == 0 and kr == 0:
                    update[...] = step
                    new[...] = weight


def kernel_body(
    normed_input,
    query_cotangent,
    value_cotangent,
    query_basis,
    value_basis,
    query_weight,
    value_weight,
    query_first,
    query_second,
    value_first,
    value_second,
):
    fs, rep, tp = lax.axis_size("fs"), lax.axis_size("rep"), lax.axis_size("tp")
    place = jnp.stack([lax.axis_index("fs"), lax.axis_index("rep")]).astype(jnp.int32)
    rows, ranks = query_weight.shape[0], query_first.shape[0]
    query_width, value_width = query_cotangent.shape[1], value_cotangent.shape[1]
    width = query_width + value_width
    total = fs * rep * rows

    def shape(*dims, dtype=F32):
        return jax.ShapeDtypeStruct(dims, dtype)

    def call(kernel, out_shape, *operands, scratch=(), outside=()):
        specs = [SMEM if operand is place else VMEM for operand in operands]
        specs = [ANY if i in outside else spec for i, spec in enumerate(specs)]
        operands = [
            pltpu.with_memory_space_constraint(operand, pltpu.HBM) if i in outside else operand
            for i, operand in enumerate(operands)
        ]
        return pl.pallas_call(
            kernel,
            out_shape=out_shape,
            in_specs=specs,
            out_specs=jax.tree.map(lambda _: VMEM, out_shape),
            scratch_shapes=scratch,
            compiler_params=PARAMS,
        )(*operands)

    weights, own = call(
        stage_kernel,
        (shape(rows, width), shape(rows + 2 * ranks, width)),
        query_weight,
        value_weight,
        query_first,
        value_first,
        query_second,
        value_second,
        scratch=[pltpu.SemaphoreType.DMA((8,))],
        outside=range(6),
    )
    plane = spread(weights, "rep")
    along = spread(own, "fs")

    operands = (normed_input, query_basis, value_basis, query_cotangent, value_cotangent)
    chunks = call(
        functools.partial(project_kernel, (fs, rep, ranks)),
        (shape(fs * ranks, width),) * rep,
        place,
        *operands,
        scratch=[pltpu.VMEM((fs * rep * ranks, width), F32)]
        + [pltpu.VMEM(operand.shape, operand.dtype) for operand in operands]
        + [pltpu.SemaphoreType.DMA((5,))],
        outside=range(1, 6),
    )
    arrived = [swap(chunks[k], "rep", k) for k in range(1, rep)]
    mine = functools.reduce(jnp.add, arrived, chunks[0])
    far = []
    for k in range(1, fs):
        cut = along[k][:rows]
        far.append(spread(cut, "rep"))
    step = 1
    while 2 * step < fs:
        arrived = swap(mine, "fs", step)
        mine = mine + arrived
        step *= 2
    other = swap(mine, "fs", step)

    *new_moments, direction = call(
        functools.partial(moments_kernel, (fs, rows, ranks, query_width)),
        (shape(ranks, query_width),) * 2
        + (shape(ranks, value_width),) * 2
        + (shape(fs * ranks, width),),
        place,
        mine,
        other,
        *along,
    )
    whole, sums = call(
        functools.partial(whole_kernel, (fs, rep, ranks, query_width)),
        (shape(fs * rep * ranks, width), shape(2, 128)),
        place,
        *spread(direction, "rep"),
    )
    if tp == 2:
        sums = sums + swap(sums, "tp", 1)
    else:
        sums = lax.psum(sums, "tp")
    products = call(
        product_kernel,
        (shape(total, query_width), shape(total, value_width)),
        whole,
        query_basis,
        value_basis,
    )
    held = plane + sum(far, [])
    entries = (fs * rep * ranks * query_width * tp, fs * rep * ranks * value_width * tp)
    query_update, value_update, query_new, value_new, query_copy, value_copy = call(
        functools.partial(finish_kernel, (fs, rep, rows, entries)),
        (shape(rows, query_width), shape(rows, value_width)) * 2
        + (shape(total, query_width, dtype=BF16), shape(total, value_width, dtype=BF16)),
        place,
        sums,
        *products,
        *held,
    )
    query_first_new, query_second_new, value_first_new, value_second_new = new_moments
    return (
        query_update,
        value_update,
        query_new,
        value_new,
        query_first_new,
        query_second_new,
        value_first_new,
        value_second_new,
        query_copy,
        value_copy,
    )


def plain_body(
    normed_input,
    query_cotangent,
    value_cotangent,
    query_basis,
    value_basis,
    query_weight,
    value_weight,
    query_first,
    query_second,
    value_first,
    value_second,
):
    fs, rep, tp = lax.axis_size("fs"), lax.axis_size("rep"), lax.axis_size("tp")
    z, r = lax.axis_index("fs"), lax.axis_index("rep")
    rows = query_weight.shape[0]
    query_width, value_width = query_cotangent.shape[1], value_cotangent.shape[1]
    width = query_width + value_width
    total = fs * rep * rows

    weights = jnp.concatenate([query_weight, value_weight], axis=1)
    copies = in_order(spread(weights, "fs"), z)
    copies = in_order(spread(copies, "rep"), r).transpose(1, 0, 2, 3).reshape(total, width)
    partial = jnp.concatenate(
        [
            parts_product(
                *split_parts(jnp.dot(normed_input, basis, preferred_element_type=F32)), cotangent
            )
            for basis, cotangent in ((query_basis, query_cotangent), (value_basis, value_cotangent))
        ],
        axis=1,
    )
    projected = lax.psum_scatter(partial, ("fs", "rep"), scatter_dimension=0, tiled=True)
    first_new, second_new, direction = moments(
        projected,
        jnp.concatenate([query_first, value_first], axis=1),
        jnp.concatenate([query_second, value_second], axis=1),
    )
    whole = lax.all_gather(direction, ("fs", "rep"), axis=0, tiled=True)
    squares = whole * whole
    sums = lax.psum(
        jnp.stack([jnp.sum(squares[:, :query_width]), jnp.sum(squares[:, query_width:])]), "tp"
    )
    outs = []
    place = (z * rep + r) * rows
    for basis, lo, hi, squared in (
        (query_basis, 0, query_width, sums[0]),
        (value_basis, query_width, width, sums[1]),
    ):
        scale = jnp.sqrt(squared / (whole.shape[0] * (hi - lo) * tp) + 1.0)
        update = jnp.dot(basis.astype(F32), whole[:, lo:hi], precision=lax.Precision.HIGHEST) / scale
        new = copies[:, lo:hi] - 0.01 * update
        outs.append(lax.dynamic_slice_in_dim(update, place, rows, 0))
        outs.append(lax.dynamic_slice_in_dim(new, place, rows, 0))
        outs.append(new.astype(BF16))
    query_update, query_new, query_copy, value_update, value_new, value_copy = outs
    return (
        query_update,
        value_update,
        query_new,
        value_new,
        first_new[:, :query_width],
        second_new[:, :query_width],
        first_new[:, query_width:],
        second_new[:, query_width:],
        query_copy,
        value_copy,
    )


def body(*operands):
    query_weight, value_weight, query_first = operands[5:8]
    fits = query_first.shape[0] % 8 == 0 and query_weight.shape[0] % 16 == 0
    fits = fits and query_weight.shape[1] % 128 == 0 and value_weight.shape[1] % 128 == 0
    if fits and lax.axis_size("fs") >= 4:
        return kernel_body(*operands)
    return plain_body(*operands)


def solution(mesh):
    rows = P(("fs", "rep"), "tp")
    in_specs = (P(("fs", "rep"), None), rows, rows, P(), P()) + (rows,) * 6
    out_specs = (rows,) * 8 + (P(None, "tp"),) * 2
    return jax.shard_map(body, mesh=mesh, in_specs=in_specs, out_specs=out_specs, check_vma=False)
```

```python
import functools

import jax
import jax.numpy as jnp
from jax import lax
from jax.experimental import pallas as pl
from jax.experimental.pallas import tpu as pltpu
from jax.sharding import PartitionSpec as P


F32, BF16 = jnp.float32, jnp.bfloat16
VMEM = pl.BlockSpec(memory_space=pltpu.VMEM)
SMEM = pl.BlockSpec(memory_space=pltpu.SMEM)
ANY = pl.BlockSpec(memory_space=pltpu.MemorySpace.HBM)
PARAMS = pltpu.CompilerParams(vmem_limit_bytes=16 * 2**20)


def swap(block, axis, mask):
    count = lax.axis_size(axis)
    pairs = [(i, i ^ mask) for i in range(count)]
    return lax.ppermute(block, axis, pairs)


def spread(block, axis):
    return [block] + [swap(block, axis, k) for k in range(1, lax.axis_size(axis))]


def in_order(blocks, own):
    stacked = jnp.stack(blocks)
    return jnp.stack(
        [lax.dynamic_index_in_dim(stacked, j ^ own, 0, keepdims=False) for j in range(len(blocks))]
    )


def split_parts(wide):
    high_part = wide.astype(BF16)
    held = lax.optimization_barrier(high_part)
    low_part = (wide - held.astype(F32)).astype(BF16)
    return (high_part, low_part)


def parts_product(high_part, low_part, cotangent):
    dims = (((0,), (0,)), ((), ()))
    first_term = lax.dot_general(high_part, cotangent, dims, preferred_element_type=F32)
    second_term = lax.dot_general(low_part, cotangent, dims, preferred_element_type=F32)
    return first_term + second_term


def moments(projected, first_old, second_old):
    first_new = 0.9 * first_old + 0.1 * projected
    second_new = 0.99 * second_old + 0.01 * projected * projected
    return (first_new, second_new, first_new / (jnp.sqrt(second_new) + 1e-08))


def aligned(start, size):
    return pl.ds(pl.multiple_of(start * size, size), size)


def stage_kernel(*refs):
    query_weight, value_weight, query_first, value_first, query_second, value_second = refs[:6]
    sources, weights, own, targets, sems = refs[6:11], refs[11], refs[12], refs[13:18], refs[18]
    rows, ranks = query_weight.shape[0], query_first.shape[0]
    query_width, width = query_weight.shape[1], weights.shape[1]
    jobs = []
    for target, left, right, low in (
        (weights, query_weight, value_weight, 0),
        (own, query_weight, value_weight, 0),
        (own, query_first, value_first, rows),
        (own, query_second, value_second, rows + ranks),
    ):
        where = pl.ds(low, left.shape[0])
        jobs.append((left, target.at[where, pl.ds(0, query_width)]))
        jobs.append((right, target.at[where, pl.ds(query_width, width - query_width)]))
    jobs.extend(zip(sources, targets))
    copies = [pltpu.make_async_copy(*job, sems.at[i]) for i, job in enumerate(jobs)]
    for copy in copies:
        copy.start()
    for copy in copies:
        copy.wait()


def project_kernel(counts, place, tokens, query_basis, value_basis, query_cot, value_cot, *refs):
    fs, rep, ranks = counts
    chunks, total = refs[:rep], refs[rep]
    r = place[1]
    query_width = query_cot.shape[1]
    for basis, cot, lo in ((query_basis, query_cot, 0), (value_basis, value_cot, query_width)):
        reduced = jnp.dot(tokens[...], basis[...], preferred_element_type=F32)
        high = reduced.astype(BF16)
        low = (reduced - high.astype(F32)).astype(BF16)
        total[:, lo : lo + cot.shape[1]] = parts_product(high, low, cot[...])
    for k in range(rep):
        for zz in range(fs):
            chunks[k][zz * ranks : (zz + 1) * ranks, :] = total[
                aligned(zz * rep + (r ^ k), ranks), :
            ]


def direction_kernel(counts, place, mine, other, *refs):
    fs, rows, ranks = counts
    blocks, direction = refs[:fs], refs[fs]
    z = place[0]
    for k in range(fs):
        where = aligned(z ^ k, ranks)
        direction[where, :] = moments(
            mine[where, :] + other[where, :],
            blocks[k][rows : rows + ranks, :],
            blocks[k][rows + ranks : rows + 2 * ranks, :],
        )[2]


def record_kernel(counts, place, mine, other, own, *refs):
    rows, ranks, query_width = counts
    query_first, query_second, value_first, value_second = refs
    where = aligned(place[0], ranks)
    first, second, _ = moments(
        mine[where, :] + other[where, :],
        own[rows : rows + ranks, :],
        own[rows + ranks : rows + 2 * ranks, :],
    )
    query_first[...] = first[:, :query_width]
    query_second[...] = second[:, :query_width]
    value_first[...] = first[:, query_width:]
    value_second[...] = second[:, query_width:]


def whole_kernel(counts, place, *refs):
    fs, rep, ranks, query_width = counts
    blocks, (whole, sums) = refs[:rep], refs[rep:]
    r = place[1]
    for k in range(rep):
        for zz in range(fs):
            whole[aligned(zz * rep + (r ^ k), ranks), :] = blocks[k][
                zz * ranks : (zz + 1) * ranks, :
            ]
    squares = whole[0:ranks, :] * whole[0:ranks, :]
    for row in range(1, fs * rep):
        part = whole[row * ranks : (row + 1) * ranks, :]
        squares = squares + part * part
    query_sum = jnp.sum(squares[:, :query_width], keepdims=True)
    value_sum = jnp.sum(squares[:, query_width:], keepdims=True)
    sums[0:1, :] = jnp.broadcast_to(query_sum, (1, sums.shape[1]))
    sums[1:2, :] = jnp.broadcast_to(value_sum, (1, sums.shape[1]))


def product_kernel(whole, query_basis, value_basis, query_product, value_product):
    query_width = query_product.shape[1]
    for basis, product, lo in (
        (query_basis, query_product, 0),
        (value_basis, value_product, query_width),
    ):
        wide = whole[:, lo : lo + product.shape[1]]
        high = wide.astype(BF16)
        low = (wide - high.astype(F32)).astype(BF16)
        product[...] = jnp.dot(basis[...], high, preferred_element_type=F32) + jnp.dot(
            basis[...], low, preferred_element_type=F32
        )


def finish_kernel(counts, pieces, place, sums, query_product, value_product, *refs):
    rep, rows, entries, blocks = counts
    sources, refs = refs[:blocks], refs[blocks:]
    z, r = place[0], place[1]
    query_width = query_product.shape[1]
    query_scale = 1.0 / jnp.sqrt(sums[0:1, 0:1] / entries[0] + 1.0)
    value_scale = 1.0 / jnp.sqrt(sums[1:2, 0:1] / entries[1] + 1.0)
    own = any(kz == 0 and kr == 0 for kz, kr, *_ in pieces)
    if own:
        query_update, value_update, query_new, value_new, query_copy, value_copy = refs[:6]
        updates, news = (query_update, value_update), (query_new, value_new)
        refs = refs[6:]
    else:
        query_copy, value_copy = refs[2:4]
        refs = refs[4:]
    query_held, value_held, sems = refs
    copies = []
    filled = 0
    for kz, kr, source, start, offset, size in pieces:
        owner = (z ^ kz) * rep + (r ^ kr)
        where = pl.ds(pl.multiple_of(owner * rows + offset, size), size)
        slot = pl.ds(filled, size)
        for i, (product, scale, lo, held, copy) in enumerate(
            (
                (query_product, query_scale, 0, query_held, query_copy),
                (value_product, value_scale, query_width, value_held, value_copy),
            )
        ):
            step = product[where, :] * scale
            old = sources[source][start : start + size, lo : lo + product.shape[1]]
            weight = old - 0.01 * step
            held[slot, :] = weight.astype(BF16)
            if kz == 0 and kr == 0:
                updates[i][...] = step
                news[i][...] = weight
            copies.append(
                pltpu.make_async_copy(held.at[slot, :], copy.at[where, :], sems.at[len(copies)])
            )
            copies[-1].start()
        filled += size
    for copy in copies:
        copy.wait()


def kernel_body(
    normed_input,
    query_cotangent,
    value_cotangent,
    query_basis,
    value_basis,
    query_weight,
    value_weight,
    query_first,
    query_second,
    value_first,
    value_second,
):
    fs, rep, tp = lax.axis_size("fs"), lax.axis_size("rep"), lax.axis_size("tp")
    place = jnp.stack([lax.axis_index("fs"), lax.axis_index("rep")]).astype(jnp.int32)
    rows, ranks = query_weight.shape[0], query_first.shape[0]
    query_width, value_width = query_cotangent.shape[1], value_cotangent.shape[1]
    width = query_width + value_width
    total = fs * rep * rows

    def shape(*dims, dtype=F32):
        return jax.ShapeDtypeStruct(dims, dtype)

    def call(kernel, out_shape, *operands, scratch=(), outside=(), outside_out=(), aliases=None):
        specs = [SMEM if operand is place else VMEM for operand in operands]
        specs = [ANY if i in outside else spec for i, spec in enumerate(specs)]
        operands = [
            pltpu.with_memory_space_constraint(operand, pltpu.HBM) if i in outside else operand
            for i, operand in enumerate(operands)
        ]
        return pl.pallas_call(
            kernel,
            out_shape=out_shape,
            in_specs=specs,
            out_specs=tuple(ANY if i in outside_out else VMEM for i in range(len(out_shape))),
            scratch_shapes=scratch,
            input_output_aliases=aliases or {},
            compiler_params=PARAMS,
        )(*operands)

    operands = (normed_input, query_basis, value_basis, query_cotangent, value_cotangent)
    weights, own, *staged = call(
        stage_kernel,
        (shape(rows, width), shape(rows + 2 * ranks, width))
        + tuple(shape(*operand.shape, dtype=operand.dtype) for operand in operands),
        query_weight,
        value_weight,
        query_first,
        value_first,
        query_second,
        value_second,
        *operands,
        scratch=[pltpu.SemaphoreType.DMA((13,))],
        outside=range(11),
    )
    query_basis, value_basis = staged[1:3]
    half = rows // 2

    def sides(block, extra=None):
        payloads = [block, block]
        if extra is not None:
            payloads = [
                jnp.concatenate([block, extra[1][half:rows]], axis=0),
                jnp.concatenate([block, extra[0][:half]], axis=0),
            ]
        return [swap(payloads[k - 1], "rep", k) for k in (1, 2)]

    plane = sides(weights)
    along = [own]
    for k in range(1, fs):
        source, mask = (along[k - 1], 1) if k % 2 and k > 1 else (own, k)
        along.append(swap(source, "fs", mask))
    chunks = call(
        functools.partial(project_kernel, (fs, rep, ranks)),
        (shape(fs * ranks, width),) * rep,
        place,
        *staged,
        scratch=[pltpu.VMEM((fs * rep * ranks, width), F32)],
    )
    arrived = [swap(chunks[k], "rep", k) for k in range(1, rep)]
    mine = functools.reduce(jnp.add, arrived, chunks[0])
    far = [plane]
    for k in range(1, fs):
        cut = along[k][:rows]
        blocks = sides(cut, plane if k == 1 else None)
        if k == fs - 1:
            blocks.append(swap(cut, "rep", 3))
        far.append(blocks)
    cross = jnp.concatenate([far[1][1][rows:], far[1][0][rows:]], axis=0)
    crosses = [swap(cross, "fs", k) for k in range(1, fs - 1)]
    step = 1
    while 2 * step < fs:
        arrived = swap(mine, "fs", step)
        mine = mine + arrived
        step *= 2
    other = swap(mine, "fs", step)

    (direction,) = call(
        functools.partial(direction_kernel, (fs, rows, ranks)),
        (shape(fs * ranks, width),),
        place,
        mine,
        other,
        *along,
    )
    wholes = spread(direction, "rep")
    new_moments = call(
        functools.partial(record_kernel, (rows, ranks, query_width)),
        (shape(ranks, query_width),) * 2 + (shape(ranks, value_width),) * 2,
        place,
        mine,
        other,
        own,
    )
    whole, sums = call(
        functools.partial(whole_kernel, (fs, rep, ranks, query_width)),
        (shape(fs * rep * ranks, width), shape(2, 128)),
        place,
        *wholes,
    )
    if tp == 2:
        sums = sums + swap(sums, "tp", 1)
    else:
        sums = lax.psum(sums, "tp")
    products = call(
        product_kernel,
        (shape(total, query_width), shape(total, value_width)),
        whole,
        query_basis,
        value_basis,
    )

    entries = (fs * rep * ranks * query_width * tp, fs * rep * ranks * value_width * tp)
    copy_shapes = (shape(total, query_width, dtype=BF16), shape(total, value_width, dtype=BF16))

    def finish(pieces, copies=None):
        sources = []
        for piece in pieces:
            if not any(piece[2] is source for source in sources):
                sources.append(piece[2])
        found = [[i for i, s in enumerate(sources) if s is piece[2]][0] for piece in pieces]
        pieces = [(p[0], p[1], i, *p[3:]) for p, i in zip(pieces, found)]
        held = sum(piece[-1] for piece in pieces)
        first = 4 + len(sources)
        kernel = functools.partial(finish_kernel, (rep, rows, entries, len(sources)), pieces)
        scratch = [
            pltpu.VMEM((held, query_width), BF16),
            pltpu.VMEM((held, value_width), BF16),
            pltpu.SemaphoreType.DMA((2 * len(pieces),)),
        ]
        if copies is None:
            shapes = (shape(rows, query_width), shape(rows, value_width)) * 2 + copy_shapes
            return call(
                kernel, shapes, place, sums, *products, *sources, scratch=scratch, outside_out=(4, 5)
            )
        return call(
            kernel,
            copy_shapes,
            place,
            sums,
            *products,
            *sources,
            *copies,
            scratch=scratch,
            outside=(first, first + 1),
            outside_out=(0, 1),
            aliases={first: 0, first + 1: 1},
        )

    early, late = [], []
    for kz in range(fs):
        group = late if kz == fs - 1 else early
        early.append((kz, 0, along[kz], 0, 0, rows))
        for kr in (1, 2):
            group.append((kz, kr, far[kz][kr - 1], 0, 0, rows))
        if kz == fs - 1:
            late.append((kz, 3, far[kz][2], 0, 0, rows))
        else:
            (late if kz == fs - 2 else early).append((kz, 3, ([cross] + crosses)[kz], 0, 0, rows))
    query_update, value_update, query_new, value_new, *copies = finish(early)
    query_copy, value_copy = finish(late, copies)
    query_first_new, query_second_new, value_first_new, value_second_new = new_moments
    return (
        query_update,
        value_update,
        query_new,
        value_new,
        query_first_new,
        query_second_new,
        value_first_new,
        value_second_new,
        query_copy,
        value_copy,
    )


def plain_body(
    normed_input,
    query_cotangent,
    value_cotangent,
    query_basis,
    value_basis,
    query_weight,
    value_weight,
    query_first,
    query_second,
    value_first,
    value_second,
):
    fs, rep, tp = lax.axis_size("fs"), lax.axis_size("rep"), lax.axis_size("tp")
    z, r = lax.axis_index("fs"), lax.axis_index("rep")
    rows = query_weight.shape[0]
    query_width, value_width = query_cotangent.shape[1], value_cotangent.shape[1]
    width = query_width + value_width
    total = fs * rep * rows

    weights = jnp.concatenate([query_weight, value_weight], axis=1)
    copies = in_order(spread(weights, "fs"), z)
    copies = in_order(spread(copies, "rep"), r).transpose(1, 0, 2, 3).reshape(total, width)
    partial = jnp.concatenate(
        [
            parts_product(
                *split_parts(jnp.dot(normed_input, basis, preferred_element_type=F32)), cotangent
            )
            for basis, cotangent in ((query_basis, query_cotangent), (value_basis, value_cotangent))
        ],
        axis=1,
    )
    projected = lax.psum_scatter(partial, ("fs", "rep"), scatter_dimension=0, tiled=True)
    first_new, second_new, direction = moments(
        projected,
        jnp.concatenate([query_first, value_first], axis=1),
        jnp.concatenate([query_second, value_second], axis=1),
    )
    whole = lax.all_gather(direction, ("fs", "rep"), axis=0, tiled=True)
    squares = whole * whole
    sums = lax.psum(
        jnp.stack([jnp.sum(squares[:, :query_width]), jnp.sum(squares[:, query_width:])]), "tp"
    )
    outs = []
    place = (z * rep + r) * rows
    for basis, lo, hi, squared in (
        (query_basis, 0, query_width, sums[0]),
        (value_basis, query_width, width, sums[1]),
    ):
        scale = jnp.sqrt(squared / (whole.shape[0] * (hi - lo) * tp) + 1.0)
        update = jnp.dot(basis.astype(F32), whole[:, lo:hi], precision=lax.Precision.HIGHEST) / scale
        new = copies[:, lo:hi] - 0.01 * update
        outs.append(lax.dynamic_slice_in_dim(update, place, rows, 0))
        outs.append(lax.dynamic_slice_in_dim(new, place, rows, 0))
        outs.append(new.astype(BF16))
    query_update, query_new, query_copy, value_update, value_new, value_copy = outs
    return (
        query_update,
        value_update,
        query_new,
        value_new,
        first_new[:, :query_width],
        second_new[:, :query_width],
        first_new[:, query_width:],
        second_new[:, query_width:],
        query_copy,
        value_copy,
    )


def body(*operands):
    query_weight, value_weight, query_first = operands[5:8]
    fits = query_first.shape[0] % 8 == 0 and query_weight.shape[0] % 16 == 0
    fits = fits and query_weight.shape[1] % 128 == 0 and value_weight.shape[1] % 128 == 0
    if fits and lax.axis_size("fs") >= 4 and lax.axis_size("rep") == 4:
        return kernel_body(*operands)
    return plain_body(*operands)


def solution(mesh):
    rows = P(("fs", "rep"), "tp")
    in_specs = (P(("fs", "rep"), None), rows, rows, P(), P()) + (rows,) * 6
    out_specs = (rows,) * 8 + (P(None, "tp"),) * 2
    return jax.shard_map(body, mesh=mesh, in_specs=in_specs, out_specs=out_specs, check_vma=False)
```

```python
import functools

import jax
import jax.numpy as jnp
from jax import lax
from jax.experimental import pallas as pl
from jax.experimental.pallas import tpu as pltpu
from jax.sharding import PartitionSpec as P


F32, BF16 = jnp.float32, jnp.bfloat16
VMEM = pl.BlockSpec(memory_space=pltpu.VMEM)
SMEM = pl.BlockSpec(memory_space=pltpu.SMEM)
ANY = pl.BlockSpec(memory_space=pltpu.MemorySpace.HBM)
PARAMS = pltpu.CompilerParams(vmem_limit_bytes=16 * 2**20)


def swap(block, axis, mask):
    count = lax.axis_size(axis)
    pairs = [(i, i ^ mask) for i in range(count)]
    return lax.ppermute(block, axis, pairs)


def spread(block, axis):
    return [block] + [swap(block, axis, k) for k in range(1, lax.axis_size(axis))]


def in_order(blocks, own):
    stacked = jnp.stack(blocks)
    return jnp.stack(
        [lax.dynamic_index_in_dim(stacked, j ^ own, 0, keepdims=False) for j in range(len(blocks))]
    )


def split_parts(wide):
    high_part = wide.astype(BF16)
    held = lax.optimization_barrier(high_part)
    low_part = (wide - held.astype(F32)).astype(BF16)
    return (high_part, low_part)


def parts_product(high_part, low_part, cotangent):
    dims = (((0,), (0,)), ((), ()))
    first_term = lax.dot_general(high_part, cotangent, dims, preferred_element_type=F32)
    second_term = lax.dot_general(low_part, cotangent, dims, preferred_element_type=F32)
    return first_term + second_term


def moments(projected, first_old, second_old):
    first_new = 0.9 * first_old + 0.1 * projected
    second_new = 0.99 * second_old + 0.01 * projected * projected
    return (first_new, second_new, first_new / (jnp.sqrt(second_new) + 1e-08))


def aligned(start, size):
    return pl.ds(pl.multiple_of(start * size, size), size)


def stage_kernel(*refs):
    query_weight, value_weight, query_first, value_first, query_second, value_second = refs[:6]
    sources, weights, own, targets, sems = refs[6:11], refs[11], refs[12], refs[13:18], refs[18]
    rows, ranks = query_weight.shape[0], query_first.shape[0]
    query_width, width = query_weight.shape[1], weights.shape[1]
    jobs = []
    for target, left, right, low in (
        (weights, query_weight, value_weight, 0),
        (own, query_weight, value_weight, 0),
        (own, query_first, value_first, rows),
        (own, query_second, value_second, rows + ranks),
    ):
        where = pl.ds(low, left.shape[0])
        jobs.append((left, target.at[where, pl.ds(0, query_width)]))
        jobs.append((right, target.at[where, pl.ds(query_width, width - query_width)]))
    jobs.extend(zip(sources, targets))
    copies = [pltpu.make_async_copy(*job, sems.at[i]) for i, job in enumerate(jobs)]
    for copy in copies:
        copy.start()
    for copy in copies:
        copy.wait()


def project_kernel(counts, place, tokens, query_basis, value_basis, query_cot, value_cot, *refs):
    fs, rep, ranks = counts
    chunks, total = refs[:rep], refs[rep]
    r = place[1]
    query_width = query_cot.shape[1]
    for basis, cot, lo in ((query_basis, query_cot, 0), (value_basis, value_cot, query_width)):
        reduced = jnp.dot(tokens[...], basis[...], preferred_element_type=F32)
        high = reduced.astype(BF16)
        low = (reduced - high.astype(F32)).astype(BF16)
        total[:, lo : lo + cot.shape[1]] = parts_product(high, low, cot[...])
    for k in range(rep):
        for zz in range(fs):
            chunks[k][zz * ranks : (zz + 1) * ranks, :] = total[
                aligned(zz * rep + (r ^ k), ranks), :
            ]


def direction_kernel(counts, place, mine, other, *refs):
    fs, rows, ranks = counts
    blocks, direction = refs[:fs], refs[fs]
    z = place[0]
    for k in range(fs):
        where = aligned(z ^ k, ranks)
        direction[where, :] = moments(
            mine[where, :] + other[where, :],
            blocks[k][rows : rows + ranks, :],
            blocks[k][rows + ranks : rows + 2 * ranks, :],
        )[2]


def whole_kernel(counts, place, *refs):
    fs, rep, ranks, query_width = counts
    blocks, (whole, sums) = refs[:rep], refs[rep:]
    r = place[1]
    for k in range(rep):
        for zz in range(fs):
            whole[aligned(zz * rep + (r ^ k), ranks), :] = blocks[k][
                zz * ranks : (zz + 1) * ranks, :
            ]
    squares = whole[0:ranks, :] * whole[0:ranks, :]
    for row in range(1, fs * rep):
        part = whole[row * ranks : (row + 1) * ranks, :]
        squares = squares + part * part
    query_sum = jnp.sum(squares[:, :query_width], keepdims=True)
    value_sum = jnp.sum(squares[:, query_width:], keepdims=True)
    sums[0:1, :] = jnp.broadcast_to(query_sum, (1, sums.shape[1]))
    sums[1:2, :] = jnp.broadcast_to(value_sum, (1, sums.shape[1]))


def product_kernel(whole, query_basis, value_basis, query_product, value_product):
    query_width = query_product.shape[1]
    for basis, product, lo in (
        (query_basis, query_product, 0),
        (value_basis, value_product, query_width),
    ):
        wide = whole[:, lo : lo + product.shape[1]]
        high = wide.astype(BF16)
        low = (wide - high.astype(F32)).astype(BF16)
        product[...] = jnp.dot(basis[...], high, preferred_element_type=F32) + jnp.dot(
            basis[...], low, preferred_element_type=F32
        )


def scales(sums, entries):
    return [1.0 / jnp.sqrt(sums[i : i + 1, 0:1] / entries[i] + 1.0) for i in range(2)]


def early_kernel(counts, pieces, place, sums, query_product, value_product, *refs):
    rep, rows, entries, blocks = counts
    sources, held = refs[:blocks], refs[blocks:]
    z, r = place[0], place[1]
    factors = scales(sums, entries)
    filled = 0
    for kz, kr, source, start, offset, size in pieces:
        owner = (z ^ kz) * rep + (r ^ kr)
        where = pl.ds(pl.multiple_of(owner * rows + offset, size), size)
        lo = 0
        for product, factor, out in zip((query_product, value_product), factors, held):
            old = sources[source][start : start + size, lo : lo + product.shape[1]]
            weight = old - 0.01 * (product[where, :] * factor)
            out[filled : filled + size, :] = weight.astype(BF16)
            lo += product.shape[1]
        filled += size


def late_kernel(counts, ready, pieces, place, sums, query_product, value_product, *refs):
    rep, rows, entries, blocks, ranks = counts
    early, sources, (mine, other) = refs[:2], refs[2 : 2 + blocks], refs[2 + blocks : 4 + blocks]
    outs, refs = refs[4 + blocks : 14 + blocks], refs[14 + blocks :]
    copy_outs, (held, staged, sems) = outs[8:], (refs[:2], refs[2:10], refs[10])
    z, r = place[0], place[1]
    query_width = query_product.shape[1]
    copies = []

    def send(source, target):
        copies.append(pltpu.make_async_copy(source, target, sems.at[len(copies)]))
        copies[-1].start()

    def target_rows(kz, kr, offset, size):
        owner = (z ^ kz) * rep + (r ^ kr)
        return pl.ds(pl.multiple_of(owner * rows + offset, size), size)

    filled = 0
    for kz, kr, _, _, offset, size in ready:
        for source, out in zip(early, copy_outs):
            send(source.at[pl.ds(filled, size), :], out.at[target_rows(kz, kr, offset, size), :])
        filled += size
    factors = scales(sums, entries)
    filled = 0
    for kz, kr, source, start, offset, size in pieces:
        where = target_rows(kz, kr, offset, size)
        lo = 0
        for i, product in enumerate((query_product, value_product)):
            step = product[where, :] * factors[i]
            weight = sources[source][start : start + size, lo : lo + product.shape[1]] - 0.01 * step
            held[i][filled : filled + size, :] = weight.astype(BF16)
            send(held[i].at[pl.ds(filled, size), :], copy_outs[i].at[where, :])
            lo += product.shape[1]
            if kz == 0 and kr == 0:
                staged[i][...] = step
                staged[2 + i][...] = weight
                send(staged[i], outs[i])
                send(staged[2 + i], outs[2 + i])
        if kz == 0 and kr == 0:
            where = aligned(z, ranks)
            first, second, _ = moments(
                mine[where, :] + other[where, :],
                sources[source][rows : rows + ranks, :],
                sources[source][rows + ranks : rows + 2 * ranks, :],
            )
            parts = (first[:, :query_width], second[:, :query_width])
            parts += (first[:, query_width:], second[:, query_width:])
            for i, part in enumerate(parts):
                staged[4 + i][...] = part
                send(staged[4 + i], outs[4 + i])
        filled += size
    for copy in copies:
        copy.wait()


def kernel_body(
    normed_input,
    query_cotangent,
    value_cotangent,
    query_basis,
    value_basis,
    query_weight,
    value_weight,
    query_first,
    query_second,
    value_first,
    value_second,
):
    fs, rep, tp = lax.axis_size("fs"), lax.axis_size("rep"), lax.axis_size("tp")
    place = jnp.stack([lax.axis_index("fs"), lax.axis_index("rep")]).astype(jnp.int32)
    rows, ranks = query_weight.shape[0], query_first.shape[0]
    query_width, value_width = query_cotangent.shape[1], value_cotangent.shape[1]
    width = query_width + value_width
    total = fs * rep * rows

    def shape(*dims, dtype=F32):
        return jax.ShapeDtypeStruct(dims, dtype)

    def call(kernel, out_shape, *operands, scratch=(), outside=(), outside_out=(), aliases=None):
        specs = [SMEM if operand is place else VMEM for operand in operands]
        specs = [ANY if i in outside else spec for i, spec in enumerate(specs)]
        operands = [
            pltpu.with_memory_space_constraint(operand, pltpu.HBM) if i in outside else operand
            for i, operand in enumerate(operands)
        ]
        return pl.pallas_call(
            kernel,
            out_shape=out_shape,
            in_specs=specs,
            out_specs=tuple(ANY if i in outside_out else VMEM for i in range(len(out_shape))),
            scratch_shapes=scratch,
            input_output_aliases=aliases or {},
            compiler_params=PARAMS,
        )(*operands)

    operands = (normed_input, query_basis, value_basis, query_cotangent, value_cotangent)
    weights, own, *staged = call(
        stage_kernel,
        (shape(rows, width), shape(rows + 2 * ranks, width))
        + tuple(shape(*operand.shape, dtype=operand.dtype) for operand in operands),
        query_weight,
        value_weight,
        query_first,
        value_first,
        query_second,
        value_second,
        *operands,
        scratch=[pltpu.SemaphoreType.DMA((13,))],
        outside=range(11),
    )
    query_basis, value_basis = staged[1:3]
    half = rows // 2

    def sides(block, extra=None):
        payloads = [block, block]
        if extra is not None:
            payloads = [
                jnp.concatenate([block, extra[1][half:rows]], axis=0),
                jnp.concatenate([block, extra[0][:half]], axis=0),
            ]
        return [swap(payloads[k - 1], "rep", k) for k in (1, 2)]

    plane = sides(weights)
    along = [own]
    for k in range(1, fs):
        source, mask = (along[k - 1], 1) if k % 2 and k > 1 else (own, k)
        along.append(swap(source, "fs", mask))
    chunks = call(
        functools.partial(project_kernel, (fs, rep, ranks)),
        (shape(fs * ranks, width),) * rep,
        place,
        *staged,
        scratch=[pltpu.VMEM((fs * rep * ranks, width), F32)],
    )
    arrived = [swap(chunks[k], "rep", k) for k in range(1, rep)]
    mine = functools.reduce(jnp.add, arrived, chunks[0])
    far = [plane]
    for k in range(1, fs):
        cut = along[k][:rows]
        blocks = sides(cut, plane if k == 1 else None)
        if k == fs - 1:
            blocks.append(swap(cut, "rep", 3))
        far.append(blocks)
    cross = jnp.concatenate([far[1][1][rows:], far[1][0][rows:]], axis=0)
    crosses = [swap(cross, "fs", k) for k in range(1, fs - 1)]
    step = 1
    while 2 * step < fs:
        arrived = swap(mine, "fs", step)
        mine = mine + arrived
        step *= 2
    other = swap(mine, "fs", step)

    (direction,) = call(
        functools.partial(direction_kernel, (fs, rows, ranks)),
        (shape(fs * ranks, width),),
        place,
        mine,
        other,
        *along,
    )
    wholes = spread(direction, "rep")
    whole, sums = call(
        functools.partial(whole_kernel, (fs, rep, ranks, query_width)),
        (shape(fs * rep * ranks, width), shape(2, 128)),
        place,
        *wholes,
    )
    if tp == 2:
        sums = sums + swap(sums, "tp", 1)
    else:
        sums = lax.psum(sums, "tp")
    products = call(
        product_kernel,
        (shape(total, query_width), shape(total, value_width)),
        whole,
        query_basis,
        value_basis,
    )

    entries = (fs * rep * ranks * query_width * tp, fs * rep * ranks * value_width * tp)

    def indexed(pieces):
        sources = []
        for piece in pieces:
            if not any(piece[2] is source for source in sources):
                sources.append(piece[2])
        found = [[i for i, s in enumerate(sources) if s is piece[2]][0] for piece in pieces]
        return sources, [(p[0], p[1], i, *p[3:]) for p, i in zip(pieces, found)]

    early, late = [], [(0, 0, own, 0, 0, rows)]
    for kz in range(fs):
        group = late if kz == fs - 1 else early
        if kz > 0:
            early.append((kz, 0, along[kz], 0, 0, rows))
        for kr in (1, 2):
            group.append((kz, kr, far[kz][kr - 1], 0, 0, rows))
        if kz == fs - 1:
            late.append((kz, 3, far[kz][2], 0, 0, rows))
        else:
            (late if kz == fs - 2 else early).append((kz, 3, ([cross] + crosses)[kz], 0, 0, rows))

    def halves(count, dtype=F32):
        return (shape(count, query_width, dtype=dtype), shape(count, value_width, dtype=dtype))

    sources, early = indexed(early)
    early_rows = sum(piece[-1] for piece in early)
    ready = call(
        functools.partial(early_kernel, (rep, rows, entries, len(sources)), early),
        halves(early_rows, BF16),
        place,
        sums,
        *products,
        *sources,
    )
    sources, late = indexed(late)
    moment_shapes = (shape(ranks, query_width),) * 2 + (shape(ranks, value_width),) * 2
    shapes = halves(rows) * 2 + moment_shapes
    late_rows = sum(piece[-1] for piece in late)
    return call(
        functools.partial(late_kernel, (rep, rows, entries, len(sources), ranks), early, late),
        shapes + halves(total, BF16),
        place,
        sums,
        *products,
        *ready,
        *sources,
        mine,
        other,
        scratch=[pltpu.VMEM(s.shape, s.dtype) for s in halves(late_rows, BF16) + shapes]
        + [pltpu.SemaphoreType.DMA((2 * len(early) + 2 * len(late) + 8,))],
        outside_out=range(10),
    )


def plain_body(
    normed_input,
    query_cotangent,
    value_cotangent,
    query_basis,
    value_basis,
    query_weight,
    value_weight,
    query_first,
    query_second,
    value_first,
    value_second,
):
    fs, rep, tp = lax.axis_size("fs"), lax.axis_size("rep"), lax.axis_size("tp")
    z, r = lax.axis_index("fs"), lax.axis_index("rep")
    rows = query_weight.shape[0]
    query_width, value_width = query_cotangent.shape[1], value_cotangent.shape[1]
    width = query_width + value_width
    total = fs * rep * rows

    weights = jnp.concatenate([query_weight, value_weight], axis=1)
    copies = in_order(spread(weights, "fs"), z)
    copies = in_order(spread(copies, "rep"), r).transpose(1, 0, 2, 3).reshape(total, width)
    partial = jnp.concatenate(
        [
            parts_product(
                *split_parts(jnp.dot(normed_input, basis, preferred_element_type=F32)), cotangent
            )
            for basis, cotangent in ((query_basis, query_cotangent), (value_basis, value_cotangent))
        ],
        axis=1,
    )
    projected = lax.psum_scatter(partial, ("fs", "rep"), scatter_dimension=0, tiled=True)
    first_new, second_new, direction = moments(
        projected,
        jnp.concatenate([query_first, value_first], axis=1),
        jnp.concatenate([query_second, value_second], axis=1),
    )
    whole = lax.all_gather(direction, ("fs", "rep"), axis=0, tiled=True)
    squares = whole * whole
    sums = lax.psum(
        jnp.stack([jnp.sum(squares[:, :query_width]), jnp.sum(squares[:, query_width:])]), "tp"
    )
    outs = []
    place = (z * rep + r) * rows
    for basis, lo, hi, squared in (
        (query_basis, 0, query_width, sums[0]),
        (value_basis, query_width, width, sums[1]),
    ):
        scale = jnp.sqrt(squared / (whole.shape[0] * (hi - lo) * tp) + 1.0)
        update = jnp.dot(basis.astype(F32), whole[:, lo:hi], precision=lax.Precision.HIGHEST) / scale
        new = copies[:, lo:hi] - 0.01 * update
        outs.append(lax.dynamic_slice_in_dim(update, place, rows, 0))
        outs.append(lax.dynamic_slice_in_dim(new, place, rows, 0))
        outs.append(new.astype(BF16))
    query_update, query_new, query_copy, value_update, value_new, value_copy = outs
    return (
        query_update,
        value_update,
        query_new,
        value_new,
        first_new[:, :query_width],
        second_new[:, :query_width],
        first_new[:, query_width:],
        second_new[:, query_width:],
        query_copy,
        value_copy,
    )


def body(*operands):
    query_weight, value_weight, query_first = operands[5:8]
    fits = query_first.shape[0] % 8 == 0 and query_weight.shape[0] % 16 == 0
    fits = fits and query_weight.shape[1] % 128 == 0 and value_weight.shape[1] % 128 == 0
    if fits and lax.axis_size("fs") >= 4 and lax.axis_size("rep") == 4:
        return kernel_body(*operands)
    return plain_body(*operands)


def solution(mesh):
    rows = P(("fs", "rep"), "tp")
    in_specs = (P(("fs", "rep"), None), rows, rows, P(), P()) + (rows,) * 6
    out_specs = (rows,) * 8 + (P(None, "tp"),) * 2
    return jax.shard_map(body, mesh=mesh, in_specs=in_specs, out_specs=out_specs, check_vma=False)
```

```python
import functools

import jax
import jax.numpy as jnp
from jax import lax
from jax.experimental import pallas as pl
from jax.experimental.pallas import tpu as pltpu
from jax.sharding import PartitionSpec as P


F32, BF16 = jnp.float32, jnp.bfloat16
VMEM = pl.BlockSpec(memory_space=pltpu.VMEM)
SMEM = pl.BlockSpec(memory_space=pltpu.SMEM)
ANY = pl.BlockSpec(memory_space=pltpu.MemorySpace.HBM)
PARAMS = pltpu.CompilerParams(vmem_limit_bytes=16 * 2**20)


def swap(block, axis, mask):
    count = lax.axis_size(axis)
    pairs = [(i, i ^ mask) for i in range(count)]
    return lax.ppermute(block, axis, pairs)


def spread(block, axis):
    return [block] + [swap(block, axis, k) for k in range(1, lax.axis_size(axis))]


def in_order(blocks, own):
    stacked = jnp.stack(blocks)
    return jnp.stack(
        [lax.dynamic_index_in_dim(stacked, j ^ own, 0, keepdims=False) for j in range(len(blocks))]
    )


def split_parts(wide):
    high_part = wide.astype(BF16)
    held = lax.optimization_barrier(high_part)
    low_part = (wide - held.astype(F32)).astype(BF16)
    return (high_part, low_part)


def parts_product(high_part, low_part, cotangent):
    dims = (((0,), (0,)), ((), ()))
    first_term = lax.dot_general(high_part, cotangent, dims, preferred_element_type=F32)
    second_term = lax.dot_general(low_part, cotangent, dims, preferred_element_type=F32)
    return first_term + second_term


def moments(projected, first_old, second_old):
    first_new = 0.9 * first_old + 0.1 * projected
    second_new = 0.99 * second_old + 0.01 * projected * projected
    return (first_new, second_new, first_new / (jnp.sqrt(second_new) + 1e-08))


def aligned(start, size):
    return pl.ds(pl.multiple_of(start * size, size), size)


def stage_kernel(*refs):
    query_weight, value_weight, query_first, value_first, query_second, value_second = refs[:6]
    sources, weights, own, targets, sems = refs[6:11], refs[11], refs[12], refs[13:18], refs[18]
    rows, ranks = query_weight.shape[0], query_first.shape[0]
    query_width, width = query_weight.shape[1], weights.shape[1]
    jobs = []
    for target, left, right, low in (
        (weights, query_weight, value_weight, 0),
        (own, query_weight, value_weight, 0),
        (own, query_first, value_first, rows),
        (own, query_second, value_second, rows + ranks),
    ):
        where = pl.ds(low, left.shape[0])
        jobs.append((left, target.at[where, pl.ds(0, query_width)]))
        jobs.append((right, target.at[where, pl.ds(query_width, width - query_width)]))
    jobs.extend(zip(sources, targets))
    copies = [pltpu.make_async_copy(*job, sems.at[i]) for i, job in enumerate(jobs)]
    for copy in copies:
        copy.start()
    for copy in copies:
        copy.wait()


def project_kernel(counts, place, tokens, query_basis, value_basis, query_cot, value_cot, *refs):
    fs, rep, ranks = counts
    chunks, total = refs[:rep], refs[rep]
    r = place[1]
    query_width = query_cot.shape[1]
    bases = jnp.concatenate([query_basis[...], value_basis[...]], axis=1)
    both = jnp.dot(tokens[...], bases, preferred_element_type=F32)
    rank = query_basis.shape[1]
    for cot, lo, at in ((query_cot, 0, 0), (value_cot, query_width, rank)):
        reduced = both[:, at : at + rank]
        high = reduced.astype(BF16)
        low = (reduced - high.astype(F32)).astype(BF16)
        total[:, lo : lo + cot.shape[1]] = lax.dot_general(
            jnp.concatenate([high, low], axis=0),
            jnp.concatenate([cot[...], cot[...]], axis=0),
            (((0,), (0,)), ((), ())),
            preferred_element_type=F32,
        )
    for k in range(rep):
        for zz in range(fs):
            chunks[k][zz * ranks : (zz + 1) * ranks, :] = total[
                aligned(zz * rep + (r ^ k), ranks), :
            ]


def direction_kernel(counts, place, mine, other, *refs):
    fs, rows, ranks = counts
    blocks, direction = refs[:fs], refs[fs]
    z = place[0]
    for k in range(fs):
        where = aligned(z ^ k, ranks)
        direction[where, :] = moments(
            mine[where, :] + other[where, :],
            blocks[k][rows : rows + ranks, :],
            blocks[k][rows + ranks : rows + 2 * ranks, :],
        )[2]


def whole_kernel(counts, place, *refs):
    fs, rep, ranks, query_width = counts
    blocks, (whole, sums) = refs[:rep], refs[rep:]
    r = place[1]
    for k in range(rep):
        for zz in range(fs):
            whole[aligned(zz * rep + (r ^ k), ranks), :] = blocks[k][
                zz * ranks : (zz + 1) * ranks, :
            ]
    squares = whole[0:ranks, :] * whole[0:ranks, :]
    for row in range(1, fs * rep):
        part = whole[row * ranks : (row + 1) * ranks, :]
        squares = squares + part * part
    query_sum = jnp.sum(squares[:, :query_width], keepdims=True)
    value_sum = jnp.sum(squares[:, query_width:], keepdims=True)
    sums[0:1, :] = jnp.broadcast_to(query_sum, (1, sums.shape[1]))
    sums[1:2, :] = jnp.broadcast_to(value_sum, (1, sums.shape[1]))


def product_kernel(whole, query_basis, value_basis, query_product, value_product):
    query_width = query_product.shape[1]
    for basis, product, lo in (
        (query_basis, query_product, 0),
        (value_basis, value_product, query_width),
    ):
        wide = whole[:, lo : lo + product.shape[1]]
        high = wide.astype(BF16)
        low = (wide - high.astype(F32)).astype(BF16)
        product[...] = jnp.dot(
            jnp.concatenate([basis[...], basis[...]], axis=1),
            jnp.concatenate([high, low], axis=0),
            preferred_element_type=F32,
        )


def scales(sums, entries):
    return [1.0 / jnp.sqrt(sums[i : i + 1, 0:1] / entries[i] + 1.0) for i in range(2)]


def early_kernel(counts, pieces, place, sums, query_product, value_product, *refs):
    rep, rows, entries, blocks, ranks = counts
    sources, (mine, other), refs = refs[:blocks], refs[blocks : blocks + 2], refs[blocks + 2 :]
    outs, copy_outs, held, staged, sems = refs[:8], refs[8:10], refs[10:12], refs[12:20], refs[20]
    z, r = place[0], place[1]
    query_width = query_product.shape[1]
    factors = scales(sums, entries)
    copies = []

    def send(source, target):
        copies.append(pltpu.make_async_copy(source, target, sems.at[len(copies)]))
        copies[-1].start()

    def form(kz, kr, source, start, offset, size):
        owner = (z ^ kz) * rep + (r ^ kr)
        where = pl.ds(pl.multiple_of(owner * rows + offset, size), size)
        lo = 0
        for i, product in enumerate((query_product, value_product)):
            step = product[where, :] * factors[i]
            weight = sources[source][start : start + size, lo : lo + product.shape[1]] - 0.01 * step
            held[i][where, :] = weight.astype(BF16)
            lo += product.shape[1]
            if kz == 0 and kr == 0:
                staged[i][...] = step
                staged[2 + i][...] = weight

    for piece in pieces:
        if piece[0] == 0:
            form(*piece)
        if piece[:2] == (0, 0):
            base = sources[piece[2]]
            where = aligned(z, ranks)
            first, second, _ = moments(
                mine[where, :] + other[where, :],
                base[rows : rows + ranks, :],
                base[rows + ranks : rows + 2 * ranks, :],
            )
            staged[4][...] = first[:, :query_width]
            staged[5][...] = second[:, :query_width]
            staged[6][...] = first[:, query_width:]
            staged[7][...] = second[:, query_width:]
            for source, target in zip(staged, outs):
                send(source, target)
    where = pl.ds(pl.multiple_of(z * rep * rows, rep * rows), rep * rows)
    for source, target in zip(held, copy_outs):
        send(source.at[where, :], target.at[where, :])
    for piece in pieces:
        if piece[0] != 0:
            form(*piece)
    for copy in copies:
        copy.wait()


def late_kernel(counts, ready, pieces, place, sums, query_product, value_product, *refs):
    rep, rows, entries, blocks = counts
    early, sources, refs = refs[:2], refs[2 : 2 + blocks], refs[4 + blocks :]
    copy_outs, held, sems = refs[:2], refs[2:4], refs[4]
    z, r = place[0], place[1]
    copies = []

    def send(source, target):
        copies.append(pltpu.make_async_copy(source, target, sems.at[len(copies)]))
        copies[-1].start()

    for kz in sorted({kz for kz, _ in ready}):
        if all((kz, kr) in ready for kr in range(rep)):
            groups = [pl.ds(pl.multiple_of((z ^ kz) * rep * rows, rep * rows), rep * rows)]
        else:
            groups = [
                aligned((z ^ kz) * rep + (r ^ kr), rows) for kr in range(rep) if (kz, kr) in ready
            ]
        for where in groups:
            for source, target in zip(early, copy_outs):
                send(source.at[where, :], target.at[where, :])
    factors = scales(sums, entries)
    filled = 0
    for kz, kr, source, start, offset, size in pieces:
        owner = (z ^ kz) * rep + (r ^ kr)
        where = pl.ds(pl.multiple_of(owner * rows + offset, size), size)
        lo = 0
        for i, product in enumerate((query_product, value_product)):
            old = sources[source][start : start + size, lo : lo + product.shape[1]]
            weight = old - 0.01 * (product[where, :] * factors[i])
            held[i][filled : filled + size, :] = weight.astype(BF16)
            send(held[i].at[pl.ds(filled, size), :], copy_outs[i].at[where, :])
            lo += product.shape[1]
        filled += size
    for copy in copies:
        copy.wait()


def kernel_body(
    normed_input,
    query_cotangent,
    value_cotangent,
    query_basis,
    value_basis,
    query_weight,
    value_weight,
    query_first,
    query_second,
    value_first,
    value_second,
):
    fs, rep, tp = lax.axis_size("fs"), lax.axis_size("rep"), lax.axis_size("tp")
    place = jnp.stack([lax.axis_index("fs"), lax.axis_index("rep")]).astype(jnp.int32)
    rows, ranks = query_weight.shape[0], query_first.shape[0]
    query_width, value_width = query_cotangent.shape[1], value_cotangent.shape[1]
    width = query_width + value_width
    total = fs * rep * rows

    def shape(*dims, dtype=F32):
        return jax.ShapeDtypeStruct(dims, dtype)

    def call(kernel, out_shape, *operands, scratch=(), outside=(), outside_out=(), aliases=None):
        specs = [SMEM if operand is place else VMEM for operand in operands]
        specs = [ANY if i in outside else spec for i, spec in enumerate(specs)]
        operands = [
            pltpu.with_memory_space_constraint(operand, pltpu.HBM) if i in outside else operand
            for i, operand in enumerate(operands)
        ]
        return pl.pallas_call(
            kernel,
            out_shape=out_shape,
            in_specs=specs,
            out_specs=tuple(ANY if i in outside_out else VMEM for i in range(len(out_shape))),
            scratch_shapes=scratch,
            input_output_aliases=aliases or {},
            compiler_params=PARAMS,
        )(*operands)

    operands = (normed_input, query_basis, value_basis, query_cotangent, value_cotangent)
    weights, own, *staged = call(
        stage_kernel,
        (shape(rows, width), shape(rows + 2 * ranks, width))
        + tuple(shape(*operand.shape, dtype=operand.dtype) for operand in operands),
        query_weight,
        value_weight,
        query_first,
        value_first,
        query_second,
        value_second,
        *operands,
        scratch=[pltpu.SemaphoreType.DMA((13,))],
        outside=range(11),
    )
    query_basis, value_basis = staged[1:3]
    half = rows // 2

    def sides(block, extra=None):
        payloads = [block, block]
        if extra is not None:
            payloads = [
                jnp.concatenate([block, extra[1][half:rows]], axis=0),
                jnp.concatenate([block, extra[0][:half]], axis=0),
            ]
        return [swap(payloads[k - 1], "rep", k) for k in (1, 2)]

    plane = sides(weights)
    along = [own]
    for k in range(1, fs):
        source, mask = (along[k - 1], 1) if k % 2 and k > 1 else (own, k)
        along.append(swap(source, "fs", mask))
    chunks = call(
        functools.partial(project_kernel, (fs, rep, ranks)),
        (shape(fs * ranks, width),) * rep,
        place,
        *staged,
        scratch=[pltpu.VMEM((fs * rep * ranks, width), F32)],
    )
    arrived = [swap(chunks[k], "rep", k) for k in range(1, rep)]
    mine = functools.reduce(jnp.add, arrived, chunks[0])
    far = [plane]
    for k in range(1, fs):
        cut = along[k][:rows]
        blocks = sides(cut, plane if k == 1 else None)
        if k == fs - 1:
            blocks.append(swap(cut, "rep", 3))
        far.append(blocks)
    cross = jnp.concatenate([far[1][1][rows:], far[1][0][rows:]], axis=0)
    crosses = [swap(cross, "fs", k) for k in range(1, fs - 1)]
    step = 1
    while 2 * step < fs:
        arrived = swap(mine, "fs", step)
        mine = mine + arrived
        step *= 2
    other = swap(mine, "fs", step)

    (direction,) = call(
        functools.partial(direction_kernel, (fs, rows, ranks)),
        (shape(fs * ranks, width),),
        place,
        mine,
        other,
        *along,
    )
    wholes = spread(direction, "rep")
    whole, sums = call(
        functools.partial(whole_kernel, (fs, rep, ranks, query_width)),
        (shape(fs * rep * ranks, width), shape(2, 128)),
        place,
        *wholes,
    )
    if tp == 2:
        sums = sums + swap(sums, "tp", 1)
    else:
        sums = lax.psum(sums, "tp")
    products = call(
        product_kernel,
        (shape(total, query_width), shape(total, value_width)),
        whole,
        query_basis,
        value_basis,
    )

    entries = (fs * rep * ranks * query_width * tp, fs * rep * ranks * value_width * tp)

    def indexed(pieces):
        sources = []
        for piece in pieces:
            if not any(piece[2] is source for source in sources):
                sources.append(piece[2])
        found = [[i for i, s in enumerate(sources) if s is piece[2]][0] for piece in pieces]
        return sources, [(p[0], p[1], i, *p[3:]) for p, i in zip(pieces, found)]

    early, late = [(0, 0, own, 0, 0, rows)], []
    for kz in range(fs):
        group = late if kz == fs - 1 else early
        if kz > 0:
            early.append((kz, 0, along[kz], 0, 0, rows))
        for kr in (1, 2):
            group.append((kz, kr, far[kz][kr - 1], 0, 0, rows))
        if kz == fs - 1:
            late.append((kz, 3, far[kz][2], 0, 0, rows))
        else:
            (late if 0 < kz else early).append((kz, 3, ([cross] + crosses)[kz], 0, 0, rows))

    def halves(count, dtype=F32):
        return (shape(count, query_width, dtype=dtype), shape(count, value_width, dtype=dtype))

    sources, early = indexed(early)
    moment_shapes = (shape(ranks, query_width),) * 2 + (shape(ranks, value_width),) * 2
    shapes = halves(rows) * 2 + moment_shapes
    *outs, query_copy, value_copy, query_ready, value_ready = call(
        functools.partial(early_kernel, (rep, rows, entries, len(sources), ranks), early),
        shapes + halves(total, BF16) * 2,
        place,
        sums,
        *products,
        *sources,
        mine,
        other,
        scratch=[pltpu.VMEM(s.shape, s.dtype) for s in shapes]
        + [pltpu.SemaphoreType.DMA((10,))],
        outside_out=range(10),
    )
    sources, late = indexed(late)
    late_rows = sum(piece[-1] for piece in late)
    ready = frozenset(piece[:2] for piece in early if piece[0] > 0)
    last = 6 + len(sources)
    copies = call(
        functools.partial(late_kernel, (rep, rows, entries, len(sources)), ready, late),
        halves(total, BF16),
        place,
        sums,
        *products,
        query_ready,
        value_ready,
        *sources,
        query_copy,
        value_copy,
        scratch=[pltpu.VMEM(s.shape, s.dtype) for s in halves(late_rows, BF16)]
        + [pltpu.SemaphoreType.DMA((2 * fs * rep,))],
        outside=(last, last + 1),
        outside_out=(0, 1),
        aliases={last: 0, last + 1: 1},
    )
    return (*outs, *copies)


def plain_body(
    normed_input,
    query_cotangent,
    value_cotangent,
    query_basis,
    value_basis,
    query_weight,
    value_weight,
    query_first,
    query_second,
    value_first,
    value_second,
):
    fs, rep, tp = lax.axis_size("fs"), lax.axis_size("rep"), lax.axis_size("tp")
    z, r = lax.axis_index("fs"), lax.axis_index("rep")
    rows = query_weight.shape[0]
    query_width, value_width = query_cotangent.shape[1], value_cotangent.shape[1]
    width = query_width + value_width
    total = fs * rep * rows

    weights = jnp.concatenate([query_weight, value_weight], axis=1)
    copies = in_order(spread(weights, "fs"), z)
    copies = in_order(spread(copies, "rep"), r).transpose(1, 0, 2, 3).reshape(total, width)
    partial = jnp.concatenate(
        [
            parts_product(
                *split_parts(jnp.dot(normed_input, basis, preferred_element_type=F32)), cotangent
            )
            for basis, cotangent in ((query_basis, query_cotangent), (value_basis, value_cotangent))
        ],
        axis=1,
    )
    projected = lax.psum_scatter(partial, ("fs", "rep"), scatter_dimension=0, tiled=True)
    first_new, second_new, direction = moments(
        projected,
        jnp.concatenate([query_first, value_first], axis=1),
        jnp.concatenate([query_second, value_second], axis=1),
    )
    whole = lax.all_gather(direction, ("fs", "rep"), axis=0, tiled=True)
    squares = whole * whole
    sums = lax.psum(
        jnp.stack([jnp.sum(squares[:, :query_width]), jnp.sum(squares[:, query_width:])]), "tp"
    )
    outs = []
    place = (z * rep + r) * rows
    for basis, lo, hi, squared in (
        (query_basis, 0, query_width, sums[0]),
        (value_basis, query_width, width, sums[1]),
    ):
        scale = jnp.sqrt(squared / (whole.shape[0] * (hi - lo) * tp) + 1.0)
        update = jnp.dot(basis.astype(F32), whole[:, lo:hi], precision=lax.Precision.HIGHEST) / scale
        new = copies[:, lo:hi] - 0.01 * update
        outs.append(lax.dynamic_slice_in_dim(update, place, rows, 0))
        outs.append(lax.dynamic_slice_in_dim(new, place, rows, 0))
        outs.append(new.astype(BF16))
    query_update, query_new, query_copy, value_update, value_new, value_copy = outs
    return (
        query_update,
        value_update,
        query_new,
        value_new,
        first_new[:, :query_width],
        second_new[:, :query_width],
        first_new[:, query_width:],
        second_new[:, query_width:],
        query_copy,
        value_copy,
    )


def body(*operands):
    query_weight, value_weight, query_first = operands[5:8]
    fits = query_first.shape[0] % 8 == 0 and query_weight.shape[0] % 16 == 0
    fits = fits and query_weight.shape[1] % 128 == 0 and value_weight.shape[1] % 128 == 0
    if fits and lax.axis_size("fs") >= 4 and lax.axis_size("rep") == 4:
        return kernel_body(*operands)
    return plain_body(*operands)


def solution(mesh):
    rows = P(("fs", "rep"), "tp")
    in_specs = (P(("fs", "rep"), None), rows, rows, P(), P()) + (rows,) * 6
    out_specs = (rows,) * 8 + (P(None, "tp"),) * 2
    return jax.shard_map(body, mesh=mesh, in_specs=in_specs, out_specs=out_specs, check_vma=False)
```
